32 devices in a mesh: grp: 2 (over y), sp: 4 (over z), tp: 4 (over x, core).
Axes of the slice: x: 2, y: 2, z: 4, core: 2. Of those that a mesh axis runs over, the one named last changes fastest.
Arguments:
- tokens: bfloat16 [4096, 4096], P(('grp', 'sp', 'tp')), parts along dimension 0, may hold values from -6 to 6
- norm_gain: float32 [4096], replicated, may hold values from 0.1 to 1.9
- query_diff: bfloat16 [4096, 2048], P('sp', 'tp'), may hold values from -1.25 to 1.25
- key_diff: bfloat16 [4096, 2048], P('sp', 'tp'), may hold values from -1.25 to 1.25
- value_diff: bfloat16 [4096, 2048], P('sp', 'tp'), may hold values from -0.09375 to 0.09375
- lam: float32 [8], P('tp'), may hold values from 0.3 to 0.8
- output_norm_gain: float32 [256], replicated, may hold values from 0.1 to 1.9
- query_win: bfloat16 [4096, 2048], P('sp', 'tp'), may hold values from -1.25 to 1.25
- keyval_win: bfloat16 [4, 4096, 256], P(None, 'sp'), may hold values from -1.25 to 1.25
- sink: float32 [16], P('tp'), may hold values from 4 to 7
- proj_diff: bfloat16 [2048, 4096], P('tp'), may hold values from -0.125 to 0.125
- proj_win: bfloat16 [2048, 4096], P('tp'), may hold values from -0.79296875 to 0.79296875
Outputs:
- mixed: bfloat16 [4096, 4096], P(('grp', 'sp', 'tp')), parts along dimension 0
The draws below stay inside these ranges and needn't reach their ends.
There are 2 independent parts, one for each index of `grp`. The reference program is written for one: setup_inputs(seed, part) draws one part's arguments, and reference() takes and returns one part's arrays. A program takes and returns all parts, laid end to end along the dimension named above; an argument that names none is the same for every part. Nothing has to cross between parts.
All inputs are finite; a program needn't handle non-finite values.
Results may differ from the reference program's by a relative error of at most 0.015.
Values may be sent and summed in bfloat16 or wider, within the bound.
A program may use at most 128 MiB of HBM per device.

```python
import math
import jax
import jax.numpy as jnp
from jax import lax

D = 4096
HEAD = 128
DIFF_HEADS = 8
WIN_HEADS = 16
KV_HEADS = 4
WINDOW = 128
VDIM = 256
SEQ = 2048


def draw_tokens(key, part):
    base = jnp.clip(jax.random.normal(key, (SEQ, D), jnp.float32), -6.0, 6.0)
    return base.astype(jnp.bfloat16)


def diff_pair(key):
    scale = 1.3 * D ** (-0.5)
    width = DIFF_HEADS * 2 * HEAD
    first = jnp.clip(jax.random.normal(jax.random.fold_in(key, 11), (D, width), jnp.float32), -4.0, 4.0) * scale
    second = jnp.clip(jax.random.normal(jax.random.fold_in(key, 12), (D, width), jnp.float32), -4.0, 4.0) * scale
    return (first, second)


def draw_query_diff(key, part):
    return diff_pair(key)[0].astype(jnp.bfloat16)


def draw_key_diff(key, part):
    return diff_pair(key)[1].astype(jnp.bfloat16)


def window_pair(key):
    scale = 1.3 * D ** (-0.5)
    keys = jnp.clip(jax.random.normal(jax.random.fold_in(key, 21), (KV_HEADS, D, HEAD), jnp.float32), -4.0, 4.0) * scale
    values = jnp.clip(jax.random.normal(jax.random.fold_in(key, 22), (KV_HEADS, D, HEAD), jnp.float32), -4.0, 4.0) * D ** (-0.5)
    queries = jnp.clip(jax.random.normal(jax.random.fold_in(key, 23), (D, WIN_HEADS * HEAD), jnp.float32), -4.0, 4.0) * scale
    return (queries, jnp.concatenate([keys, values], axis=2))


def draw_query_win(key, part):
    return window_pair(key)[0].astype(jnp.bfloat16)


def draw_keyval_win(key, part):
    return window_pair(key)[1].astype(jnp.bfloat16)


def shard_levels(rng, dims, split, least, top_value):
    level = 1.0
    for position, parts in split:
        steps = jax.random.uniform(jax.random.fold_in(jax.random.fold_in(rng, 6), position), (parts,), jnp.float32, least / len(split), top_value / len(split))
        level = level * jnp.repeat(jnp.exp(steps), dims[position] // parts).reshape((-1,) + (1,) * (len(dims) - 1 - position))
    return level


def scatter_about(rng, dims, scale, limit, shards=(), kind=jnp.bfloat16):
    values = scale * jax.random.normal(rng, dims, jnp.float32)
    if shards:
        values = values * shard_levels(rng, dims, shards, -0.22, 0.18)
    return jnp.clip(values, -limit, limit).astype(kind)


def setup_inputs(seed: int = 0, part: int = 0) -> dict:
    key_of = jax.random.split(jax.random.key(seed), 13)
    part_splits = jax.random.split(jax.random.fold_in(key_of[12], part), 13)
    return {
        "tokens": draw_tokens(jax.random.fold_in(jax.random.fold_in(key_of[12], part), 71), part),
        "norm_gain": jnp.clip(1.0 + 0.18 * jax.random.normal(key_of[1], (D,), jnp.float32), 0.1, 1.9),
        "query_diff": draw_query_diff(jax.random.fold_in(key_of[12], 71), part),
        "key_diff": draw_key_diff(jax.random.fold_in(key_of[12], 71), part),
        "value_diff": scatter_about(key_of[4], (D, DIFF_HEADS * VDIM), D ** -0.5, 0.09375, ((0, 4), (1, 4))),
        "lam": jnp.clip(0.3 + 0.5 * jax.random.uniform(key_of[5], (DIFF_HEADS,), jnp.float32) ** shard_levels(key_of[5], (DIFF_HEADS,), ((0, 4),), -0.2, 0.2), 0.3, 0.8),
        "output_norm_gain": jnp.clip(1.0 + 0.18 * jax.random.normal(key_of[6], (VDIM,), jnp.float32), 0.1, 1.9),
        "query_win": draw_query_win(jax.random.fold_in(key_of[12], 71), part),
        "keyval_win": draw_keyval_win(jax.random.fold_in(key_of[12], 71), part),
        "sink": jnp.clip(4.0 + 3.0 * jax.random.uniform(key_of[9], (WIN_HEADS,), jnp.float32) ** shard_levels(key_of[9], (WIN_HEADS,), ((0, 4),), -0.2, 0.2), 4.0, 7.0),
        "proj_diff": scatter_about(key_of[10], (DIFF_HEADS * VDIM, D), (DIFF_HEADS * VDIM) ** -0.5, 0.125, ((0, 4),)),
        "proj_win": scatter_about(key_of[11], (WIN_HEADS * HEAD, D), (6 * (WIN_HEADS * HEAD) ** -0.5), 0.79296875, ((0, 4),)),
    }


EPS = 1e-06

def root_mean_square_rows(values, gain):
    return values * lax.rsqrt(lax.optimization_barrier(jnp.mean(values * values, axis=-1, keepdims=True)) + EPS) * gain

def reference(tokens, norm_gain, query_diff, key_diff, value_diff, lam, output_norm_gain, query_win, keyval_win, sink, proj_diff, proj_win):
    seq = tokens.shape[0]
    normed = root_mean_square_rows(tokens.astype(jnp.float32), norm_gain).astype(jnp.bfloat16)

    def project(weight):
        return jnp.dot(normed, weight, preferred_element_type=jnp.float32).astype(jnp.bfloat16)
    q_diff = project(query_diff).reshape(seq, DIFF_HEADS, 2, HEAD)
    k_diff = project(key_diff).reshape(seq, DIFF_HEADS, 2, HEAD)
    v_diff = project(value_diff).reshape(seq, DIFF_HEADS, VDIM)
    q_win = project(query_win).reshape(seq, WIN_HEADS, HEAD)
    kv_win = jnp.stack([project(keyval_win[g]) for g in range(KV_HEADS)], axis=1)
    scale = HEAD ** (-0.5)
    qblock = math.gcd(seq, 512)

    def diff_head(args):
        q_head, k_head, v_head, lambda_head = args

        def one_block(q_rows):
            output_list = []
            for m in range(2):
                scores = jnp.dot(q_rows[:, m], k_head[:, m].T, preferred_element_type=jnp.float32) * scale
                top = lax.optimization_barrier(jnp.max(scores, axis=-1, keepdims=True))
                expo = jnp.exp(scores - top)
                total = lax.optimization_barrier(jnp.sum(expo, axis=-1, keepdims=True))
                output_list.append(jnp.dot(expo.astype(jnp.bfloat16), v_head, preferred_element_type=jnp.float32) / total)
            difference_output = output_list[0] - lambda_head * output_list[1]
            return root_mean_square_rows(difference_output, output_norm_gain).astype(jnp.bfloat16)
        result = lax.map(one_block, q_head.reshape(seq // qblock, qblock, 2, HEAD))
        return result.reshape(seq, VDIM)
    differential_output = lax.map(diff_head, (jnp.transpose(q_diff, (1, 0, 2, 3)), jnp.transpose(k_diff, (1, 0, 2, 3)), jnp.transpose(v_diff, (1, 0, 2)), lam))
    differential_output = jnp.transpose(differential_output, (1, 0, 2)).reshape(seq, DIFF_HEADS * VDIM)
    group = WIN_HEADS // KV_HEADS
    nblocks = seq // WINDOW
    q_blocks = q_win.reshape(nblocks, WINDOW, KV_HEADS, group, HEAD).astype(jnp.float32)
    padded = jnp.pad(kv_win, ((WINDOW, WINDOW), (0, 0), (0, 0))).reshape(nblocks + 2, WINDOW, KV_HEADS, 2 * HEAD)
    band = jnp.concatenate([padded[:-2], padded[1:-1], padded[2:]], axis=1).astype(jnp.float32)
    scores = jnp.einsum('nqgrd,nkgd->ngrqk', q_blocks, band[..., :HEAD]) * scale
    q_index = jnp.arange(WINDOW, dtype=jnp.int32)
    k_index = jnp.arange(3 * WINDOW, dtype=jnp.int32)
    offset = k_index[None, :] - WINDOW - q_index[:, None]
    key_pos = jnp.arange(nblocks, dtype=jnp.int32)[:, None] * WINDOW - WINDOW + k_index[None, :]
    valid = (jnp.abs(offset) <= WINDOW)[None] & ((key_pos >= 0) & (key_pos < seq))[:, None, :]
    scores = jnp.where(valid[:, None, None], scores, -jnp.inf)
    sink_logit = sink.reshape(KV_HEADS, group)[:, :, None, None]
    top = jnp.maximum(lax.optimization_barrier(jnp.max(scores, axis=-1, keepdims=True)), sink_logit)
    expo = jnp.exp(scores - top)
    weights = expo / (lax.optimization_barrier(jnp.sum(expo, axis=-1, keepdims=True)) + jnp.exp(sink_logit - top))
    weights = weights.astype(jnp.bfloat16).astype(jnp.float32)
    y_win = jnp.einsum('ngrqk,nkgd->nqgrd', weights, band[..., HEAD:]).astype(jnp.bfloat16)
    y_win = y_win.reshape(seq, WIN_HEADS * HEAD)
    total = jnp.dot(differential_output, proj_diff, preferred_element_type=jnp.float32)
    total = total + jnp.dot(y_win, proj_win, preferred_element_type=jnp.float32)
    return total.astype(jnp.bfloat16)
```

```python
import math

import jax
import jax.numpy as jnp
from jax import lax
from jax.experimental import pallas as pl
from jax.experimental.pallas import tpu as pltpu
from jax.sharding import PartitionSpec as P


HEAD = 128
WIN_HEADS = 16
KV_HEADS = 4
WINDOW = 128
VDIM = 256


EPS = 1e-06


def padded_2(x, sides, width):
    for axis, dim in sides:
        devices, length = (lax.axis_size(axis), x.shape[dim])
        up = [(i, (i + 1) % devices) for i in range(devices - 1)]
        down = [(j, i) for i, j in up]
        last = lax.slice_in_dim(x, length - width, length, axis=dim)
        first = lax.slice_in_dim(x, 0, width, axis=dim)
        before = lax.ppermute(last, axis, up)
        after = lax.ppermute(first, axis, down)
        x = jnp.concatenate([before, x, after], axis=dim)
    return x


def root_mean_square_rows(values, gain):
    return values * lax.rsqrt(jnp.mean(values * values, axis=-1, keepdims=True) + EPS) * gain


def shifted(x, axis, by):
    n = lax.axis_size(axis)
    return lax.ppermute(x, axis, [(i, (i + by) % n) for i in range(n)])


def shift_chip(x, by):
    n = lax.axis_size("tp")
    return lax.ppermute(x, "tp", [(i, (i + 2 * by) % n) for i in range(n)])


def swap_core(x):
    n = lax.axis_size("tp")
    return lax.ppermute(x, "tp", [(i, i ^ 1) for i in range(n)])


def gather_tp(x, axis):
    tp = lax.axis_size("tp")
    chips = tp // 2
    me = lax.axis_index("tp")
    mine = [x] + [shift_chip(x, r) for r in range(1, chips)]
    theirs = [swap_core(piece) for piece in mine]
    out = jnp.zeros(x.shape[:axis] + (tp,) + x.shape[axis:], x.dtype)
    for r in range(chips):
        at = (me - 2 * r) % tp
        out = lax.dynamic_update_slice_in_dim(out, jnp.expand_dims(mine[r], axis), at, axis)
        out = lax.dynamic_update_slice_in_dim(out, jnp.expand_dims(theirs[r], axis), at ^ 1, axis)
    return out


def scatter_tp(x):
    tp = lax.axis_size("tp")
    chips = tp // 2
    me = lax.axis_index("tp")
    core, chip = me % 2, me // 2
    x = x.reshape(chips, 2, x.shape[0] // tp, x.shape[1])
    away = lax.dynamic_index_in_dim(x, 1 - core, 1, keepdims=False).astype(jnp.bfloat16)
    keep = lax.dynamic_index_in_dim(x, core, 1, keepdims=False)
    both = keep + swap_core(away).astype(jnp.float32)
    total = lax.dynamic_index_in_dim(both, chip, 0, keepdims=False)
    for r in range(1, chips):
        sent = lax.dynamic_index_in_dim(both, (chip + r) % chips, 0, keepdims=False)
        total = total + shift_chip(sent.astype(jnp.bfloat16), r).astype(jnp.float32)
    return total.astype(jnp.bfloat16)


def diff_kernel(lam_ref, q_ref, k_ref, v_ref, gain_ref, o_ref):
    factor = HEAD ** (-0.5) * math.log2(math.e)
    maps = []
    for m in range(2):
        cols = slice(m * HEAD, (m + 1) * HEAD)
        scores = lax.dot_general(
            q_ref[:, cols], k_ref[:, cols], (((1,), (1,)), ((), ())),
            preferred_element_type=jnp.float32,
        )
        top = jnp.max(scores, axis=-1, keepdims=True)
        expo = jnp.exp2((scores - top) * factor)
        total = jnp.sum(expo, axis=-1, keepdims=True)
        out = jnp.dot(expo.astype(jnp.bfloat16), v_ref[...], preferred_element_type=jnp.float32)
        maps.append(out / total)
    d = maps[0] - lam_ref[pl.program_id(0)] * maps[1]
    d = d * lax.rsqrt(jnp.mean(d * d, axis=-1, keepdims=True) + EPS) * gain_ref[...]
    o_ref[...] = d.astype(jnp.bfloat16)


def diff_attention(q, kv, lam, gain):
    tok, rows, heads = q.shape[0], kv.shape[0], lam.shape[0]
    tile = math.gcd(tok, max(128, 524288 // rows))
    return pl.pallas_call(
        diff_kernel,
        grid=(heads, tok // tile),
        in_specs=[
            pl.BlockSpec(memory_space=pltpu.SMEM),
            pl.BlockSpec((tile, 2 * HEAD), lambda h, i: (i, h)),
            pl.BlockSpec((rows, 2 * HEAD), lambda h, i: (0, h)),
            pl.BlockSpec((rows, VDIM), lambda h, i: (0, heads + h)),
            pl.BlockSpec((1, VDIM), lambda h, i: (0, 0)),
        ],
        out_specs=pl.BlockSpec((tile, VDIM), lambda h, i: (i, h)),
        out_shape=jax.ShapeDtypeStruct((tok, heads * VDIM), jnp.bfloat16),
        cost_estimate=pl.CostEstimate(
            flops=heads * tok * rows * 2 * 2 * (HEAD + VDIM),
            bytes_accessed=2 * (q.size * 2 + kv.size),
            transcendentals=heads * 2 * tok * rows,
        ),
    )(lam, q, kv, kv, gain.reshape(1, VDIM))


def body(
    tokens,
    norm_gain,
    query_diff,
    key_diff,
    value_diff,
    lam,
    output_norm_gain,
    query_win,
    keyval_win,
    sink,
    proj_diff,
    proj_win,
):
    bf16, f32 = jnp.bfloat16, jnp.float32
    normed = root_mean_square_rows(tokens.astype(f32), norm_gain).astype(bf16)
    heads_win = sink.shape[0]
    group = WIN_HEADS // KV_HEADS
    n = lax.axis_size("sp")
    me = lax.axis_index("sp")
    parts = lax.axis_size("grp")
    part = lax.axis_index("grp")
    local, width = normed.shape
    depth = width // n
    tok = local * lax.axis_size("tp")

    slabs = normed.reshape(local, n, depth)
    across = jnp.zeros((n, local, depth), bf16)
    own = lax.dynamic_index_in_dim(slabs, me, 1, keepdims=True)
    across = lax.dynamic_update_slice_in_dim(across, jnp.swapaxes(own, 0, 1), me, 0)
    for r in range(1, n):
        sent = lax.dynamic_index_in_dim(slabs, (me + r) % n, 1, keepdims=False)
        got = shifted(sent, "sp", r)
        across = lax.dynamic_update_slice_in_dim(across, got[None], (me - r) % n, 0)

    kv_index = lax.axis_index("tp") * heads_win // group
    kv_local = lax.dynamic_index_in_dim(keyval_win, kv_index, 0, keepdims=False)
    stacked = jnp.concatenate([query_diff, query_win, kv_local], axis=1)
    share = stacked.shape[1] // parts
    half = lax.dynamic_slice_in_dim(stacked, part * share, share, axis=1)
    across, half = lax.optimization_barrier((across, half))

    pieces = [shifted(half, "sp", r) for r in range(1, n)]
    all_rows = gather_tp(across, 1).reshape(n * tok, depth)
    rows_all = gather_tp(normed, 0).reshape(tok, width)
    kv_part = jnp.concatenate(
        [
            jnp.dot(all_rows, key_diff, preferred_element_type=f32).astype(bf16),
            jnp.dot(all_rows, value_diff, preferred_element_type=f32).astype(bf16),
        ],
        axis=1,
    )
    kv = lax.psum_scatter(kv_part, "sp", scatter_dimension=0, tiled=True)
    kv = lax.all_gather(kv, "sp", axis=0, tiled=True)

    own_rows = lax.dynamic_slice_in_dim(rows_all, me * depth, depth, axis=1)
    own_sum = jnp.dot(own_rows, stacked, preferred_element_type=f32)
    sums = [jnp.zeros((tok, share), f32) for _ in range(parts)]
    for r in range(1, n):
        piece = pieces[r - 1]
        rows = lax.dynamic_slice_in_dim(rows_all, (me - r) % n * depth, depth, axis=1)
        for j in range(parts):
            block = piece if j == 0 else shifted(piece, "grp", j)
            sums[j] = sums[j] + jnp.dot(rows, block, preferred_element_type=f32)
    ordered = jnp.stack(sums)
    ordered = jnp.concatenate(
        [
            lax.dynamic_index_in_dim(ordered, (part - b) % parts, 0, keepdims=False)
            for b in range(parts)
        ],
        axis=1,
    )
    projected = (own_sum + ordered).astype(bf16)
    first = query_diff.shape[1]
    second = first + query_win.shape[1]
    q_diff, q_win, kv_win = projected[:, :first], projected[:, first:second], projected[:, second:]
    scale = HEAD ** (-0.5)
    padded = padded_2(kv_win, (("sp", 0),), WINDOW)
    nblocks = tok // WINDOW
    blocks = padded.reshape(nblocks + 2, WINDOW, 2 * HEAD)
    band = jnp.concatenate([blocks[:-2], blocks[1:-1], blocks[2:]], axis=1)
    q_blocks = q_win.reshape(nblocks, WINDOW, heads_win, HEAD)
    scores = (
        jnp.einsum("nqhd,nkd->nhqk", q_blocks, band[..., :HEAD], preferred_element_type=jnp.float32)
        * scale
    )
    q_index = jnp.arange(WINDOW)
    k_index = jnp.arange(3 * WINDOW)
    relative = k_index[None, :] - WINDOW - q_index[:, None]
    first_key = lax.axis_index("sp") * tok - WINDOW
    key_pos = first_key + jnp.arange(nblocks)[:, None] * WINDOW + k_index[None, :]
    inside = (key_pos >= 0) & (key_pos < tok * lax.axis_size("sp"))
    valid = (jnp.abs(relative) <= WINDOW)[None] & inside[:, None, :]
    scores = jnp.where(valid[:, None], scores, -jnp.inf)
    sink_logit = sink[None, :, None, None]
    top_win = jnp.maximum(jnp.max(scores, axis=-1, keepdims=True), sink_logit)
    expo = jnp.exp(scores - top_win)
    weights = expo / (jnp.sum(expo, axis=-1, keepdims=True) + jnp.exp(sink_logit - top_win))
    y_win = jnp.einsum(
        "nhqk,nkd->nqhd",
        weights.astype(jnp.bfloat16),
        band[..., HEAD:],
        preferred_element_type=jnp.float32,
    ).astype(jnp.bfloat16)
    y_win = y_win.reshape(tok, heads_win * HEAD)
    summed = jnp.dot(y_win, proj_win, preferred_element_type=jnp.float32)
    differential_output = diff_attention(q_diff, kv, lam, output_norm_gain)
    summed = summed + jnp.dot(differential_output, proj_diff, preferred_element_type=jnp.float32)
    return scatter_tp(summed)


def solution(mesh):
    placed = (
        P(("grp", "sp", "tp"), None),
        P(),
        P("sp", "tp"),
        P("sp", "tp"),
        P("sp", "tp"),
        P("tp"),
        P(),
        P("sp", "tp"),
        P(None, "sp", None),
        P("tp"),
        P("tp", None),
        P("tp", None),
    )
    return jax.shard_map(
        body, mesh=mesh, in_specs=placed, out_specs=P(("grp", "sp", "tp"), None), check_vma=False
    )
```
